32 devices in a mesh: sp: 16 (over z, y, core), tp: 2 (over x).
Axes of the slice: x: 2, y: 2, z: 4, core: 2. Of those that a mesh axis runs over, the one named last changes fastest.
Arguments:
- query_latent: bfloat16 [4096, 1024], P('sp'), may hold values from -6 to 6
- shared_latent: bfloat16 [4096, 512], P('sp'), may hold values from -25 to 25
- rotary_key: bfloat16 [4096, 64], P('sp'), may hold values from -300 to 300
- document_start: int32 [4096], P('sp'), may hold values from 0 to 4095, as said below
- query_gain: float32 [1024], replicated, may hold values from 0.1 to 1.9
- shared_gain: float32 [512], replicated, may hold values from 0.1 to 1.9
- content_weight: bfloat16 [1024, 2048], P(None, 'tp'), may hold values from -0.1875 to 0.1875
- rotary_weight: bfloat16 [1024, 1024], P(None, 'tp'), may hold values from -0.1875 to 0.1875
- key_weight: bfloat16 [512, 2048], P(None, 'tp'), may hold values from -0.25 to 0.25
- value_weight: bfloat16 [512, 2048], P(None, 'tp'), may hold values from -0.25 to 0.25
- output_weight: bfloat16 [2048, 4096], P('tp'), may hold values from -0.125 to 0.125
Outputs:
- mixed: bfloat16 [4096, 4096], P('sp')
The draws below stay inside these ranges and needn't reach their ends.
Inputs may be any that keep to these rules, and one draw needn't show every extreme that they name: `document_start`: each position holds the first position of its document; documents are runs of 1 to 1792 consecutive positions and one of them has exactly 1792; the values never fall.
All inputs are finite; a program needn't handle non-finite values.
Results may differ from the reference program's by a relative error of at most 0.038.
The reference program's roundings to bfloat16 on the way count: a program that leaves them out, or rounds other values in their place, can miss the bound.
Values may be sent and summed in bfloat16 or wider, within the bound.
A program may use at most 64 MiB of HBM per device.

```python
import jax
import jax.numpy as jnp
from jax import lax

MODEL = 4096
HEADS = 16
CONTENT = 128
ROTARY = 64
VALUE_DIM = 128
QUERY_RANK = 1024
SHARED_RANK = 512
SPAN = 8
TOK_DEV = 256
TOKENS = 4096
DOC_MOST = 1792
HEADS_DEV = 8


def draw_shared_latent(key, part):
    first_key = jax.random.fold_in(key, 11)
    second_key = jax.random.fold_in(key, 12)
    blocks = TOKENS // TOK_DEV
    base = jnp.clip(jax.random.normal(first_key, (TOKENS, SHARED_RANK), jnp.float32), -6.0, 6.0)
    means = 0.8 * jnp.clip(jax.random.normal(second_key, (blocks, SHARED_RANK), jnp.float32), -6.0, 6.0)
    result = base + jnp.repeat(means, TOK_DEV, axis=0)
    return jnp.clip(result, -25.0, 25.0).astype(jnp.bfloat16)


def draw_rotary_key(key, part):
    first_key = jax.random.fold_in(key, 21)
    result = jnp.clip(jax.random.normal(first_key, (TOKENS, ROTARY), jnp.float32), -6.0, 6.0)
    return jnp.clip(result, -300.0, 300.0).astype(jnp.bfloat16)


def draw_document_start(key, part):
    first_key = jax.random.fold_in(key, 31)
    second_key = jax.random.fold_in(key, 32)
    positions = jnp.arange(TOKENS, dtype=jnp.int32)
    lengths = jax.random.randint(first_key, (TOKENS,), 1, DOC_MOST + 1, dtype=jnp.int32)
    opening = jax.random.randint(second_key, (), 1, TOK_DEV, dtype=jnp.int32)
    lengths = jnp.where(positions == 0, opening, jnp.where(positions == 1, DOC_MOST, lengths))
    starts = jnp.cumsum(lengths).astype(jnp.int32) - lengths
    document = jnp.searchsorted(starts, positions, side='right') - 1
    result = starts[document].astype(jnp.int32)
    return jnp.where(positions == TOKENS - 1, positions, result).astype(jnp.int32)


def block_scale(key, shape, shards, low, largest):
    factor_of, own = 1.0, jax.random.fold_in(key, 6)
    for position, shards_of in shards:
        draws = jnp.exp(jax.random.uniform(jax.random.fold_in(own, position), (shards_of,), jnp.float32, low / len(shards), largest / len(shards)))
        factor_of = factor_of * jnp.repeat(draws, shape[position] // shards_of).reshape([-1 if axis == position else 1 for axis in range(len(shape))])
    return factor_of


def bell_draw(rng, extent, scale, bound, pieces=(), held_as=jnp.bfloat16):
    values = jax.random.normal(rng, extent, jnp.float32) * scale
    if len(pieces) > 0:
        values = block_scale(rng, extent, pieces, -0.22, 0.18) * values
    return jnp.clip(values, min=-bound, max=bound).astype(held_as)


def setup_inputs(seed: int = 0) -> dict:
    arg_keys = jax.random.split(jax.random.key(seed), 12)
    return {
        "query_latent": bell_draw(arg_keys[0], (TOKENS, QUERY_RANK), 1.0, 6.0, ((0, 16),)),
        "shared_latent": draw_shared_latent(jax.random.fold_in(arg_keys[11], 71), 0),
        "rotary_key": draw_rotary_key(jax.random.fold_in(arg_keys[11], 71), 0),
        "document_start": draw_document_start(jax.random.fold_in(arg_keys[11], 71), 0),
        "query_gain": jnp.clip(1.0 + 0.18 * jax.random.normal(arg_keys[4], (QUERY_RANK,), jnp.float32), 0.1, 1.9),
        "shared_gain": jnp.clip(1.0 + 0.18 * jax.random.normal(arg_keys[5], (SHARED_RANK,), jnp.float32), 0.1, 1.9),
        "content_weight": bell_draw(arg_keys[6], (QUERY_RANK, HEADS * CONTENT), QUERY_RANK ** -0.5, 0.1875, ((1, 2),)),
        "rotary_weight": bell_draw(arg_keys[7], (QUERY_RANK, HEADS * ROTARY), QUERY_RANK ** -0.5, 0.1875, ((1, 2),)),
        "key_weight": bell_draw(arg_keys[8], (SHARED_RANK, HEADS * CONTENT), SHARED_RANK ** -0.5, 0.25, ((1, 2),)),
        "value_weight": bell_draw(arg_keys[9], (SHARED_RANK, HEADS * VALUE_DIM), SHARED_RANK ** -0.5, 0.25, ((1, 2),)),
        "output_weight": bell_draw(arg_keys[10], (HEADS * VALUE_DIM, MODEL), (HEADS * VALUE_DIM) ** -0.5, 0.125, ((0, 2),)),
    }


norm_eps = 1e-06
rope_theta = 10000.0
masked_score = -1e+30

def rms_scale(latent, scaling):
    entries = latent.astype(jnp.float32)
    scaled = entries * lax.rsqrt(lax.optimization_barrier(jnp.mean(entries * entries, axis=-1, keepdims=True)) + norm_eps)
    return (scaled * scaling.astype(jnp.float32)).astype(jnp.bfloat16)

def rotate(entries, places):
    width = entries.shape[-1]
    halfway = width // 2
    frequency = 1.0 / rope_theta ** (jnp.arange(0, width, 2, dtype=jnp.float32) / width)
    angles = places.astype(jnp.float32)[:, None] * frequency[None, :]
    target = (angles.shape[0],) + (1,) * (entries.ndim - 2) + (halfway,)
    cosine_table = jnp.cos(angles).reshape(target)
    sine_table = jnp.sin(angles).reshape(target)
    leading = entries[..., :halfway]
    trailing = entries[..., halfway:]
    return jnp.concatenate([leading * cosine_table - trailing * sine_table, leading * sine_table + trailing * cosine_table], axis=-1)

def reference(query_latent, shared_latent, rotary_key, document_start, query_gain, shared_gain, content_weight, rotary_weight, key_weight, value_weight, output_weight):
    places = jnp.arange(TOKENS, dtype=jnp.int32)
    query_norm = rms_scale(query_latent, query_gain)
    shared_norm = rms_scale(shared_latent, shared_gain)
    key_turn = rotate(rotary_key.astype(jnp.float32), places).astype(jnp.bfloat16)
    query_content = jnp.dot(query_norm, content_weight, preferred_element_type=jnp.float32).astype(jnp.bfloat16).reshape(TOKENS, HEADS, CONTENT)
    query_raw = jnp.dot(query_norm, rotary_weight, preferred_element_type=jnp.float32).reshape(TOKENS, HEADS, ROTARY)
    query_turn = rotate(query_raw, places).astype(jnp.bfloat16)
    head_keys = jnp.dot(shared_norm, key_weight, preferred_element_type=jnp.float32).astype(jnp.bfloat16).reshape(TOKENS, HEADS, CONTENT)
    head_values = jnp.dot(shared_norm, value_weight, preferred_element_type=jnp.float32).astype(jnp.bfloat16).reshape(TOKENS, HEADS, VALUE_DIM)
    leading_pad = (SPAN - 1) * TOK_DEV
    window = SPAN * TOK_DEV
    padded_keys = jnp.pad(head_keys, ((leading_pad, 0), (0, 0), (0, 0)))
    padded_values = jnp.pad(head_values, ((leading_pad, 0), (0, 0), (0, 0)))
    padded_turn = jnp.pad(key_turn, ((leading_pad, 0), (0, 0)))
    score_scale = (CONTENT + ROTARY) ** (-0.5)

    def attend(block):
        opening = (block * TOK_DEV).astype(jnp.int32)
        block_content = lax.dynamic_slice_in_dim(query_content, opening, TOK_DEV, 0).astype(jnp.float32)
        block_turn = lax.dynamic_slice_in_dim(query_turn, opening, TOK_DEV, 0).astype(jnp.float32)
        block_starts = lax.dynamic_slice_in_dim(document_start, opening, TOK_DEV, 0)
        window_keys = lax.dynamic_slice_in_dim(padded_keys, opening, window, 0).astype(jnp.float32)
        window_values = lax.dynamic_slice_in_dim(padded_values, opening, window, 0).astype(jnp.float32)
        window_turn = lax.dynamic_slice_in_dim(padded_turn, opening, window, 0).astype(jnp.float32)
        key_places = opening - leading_pad + jnp.arange(window, dtype=jnp.int32)
        query_places = opening + jnp.arange(TOK_DEV, dtype=jnp.int32)
        scores = jnp.einsum('qhd,khd->hqk', block_content, window_keys) + jnp.einsum('qhr,kr->hqk', block_turn, window_turn)
        visible = (key_places[None, :] >= block_starts[:, None]) & (key_places[None, :] <= query_places[:, None])
        scores = jnp.where(visible[None], scores * score_scale, masked_score)
        highest = lax.optimization_barrier(jnp.max(scores, axis=-1, keepdims=True))
        weights = jnp.exp(scores - highest)
        denominator = lax.optimization_barrier(jnp.sum(weights, axis=-1))
        weights_low = weights.astype(jnp.bfloat16).astype(jnp.float32)
        summed = jnp.einsum('hqk,khd->qhd', weights_low, window_values)
        attended = summed / jnp.transpose(denominator)[:, :, None]
        return attended.astype(jnp.bfloat16).reshape(TOK_DEV, HEADS * VALUE_DIM)
    blocks = jnp.arange(TOKENS // TOK_DEV, dtype=jnp.int32)
    attended = lax.map(attend, blocks).reshape(TOKENS, HEADS * VALUE_DIM)
    group_width = HEADS_DEV * VALUE_DIM
    mixed = jnp.zeros((TOKENS, MODEL), jnp.float32)
    for group in range(HEADS // HEADS_DEV):
        columns = attended[:, group * group_width:(group + 1) * group_width]
        matching = output_weight[group * group_width:(group + 1) * group_width]
        group_term = jnp.dot(columns, matching, preferred_element_type=jnp.float32).astype(jnp.bfloat16)
        mixed = mixed + group_term.astype(jnp.float32)
    return mixed.astype(jnp.bfloat16)
```

```python
import functools

import jax
import jax.numpy as jnp
import numpy as np
from jax import lax
from jax.experimental import pallas as pl
from jax.experimental.pallas import tpu as pltpu
from jax.sharding import PartitionSpec as P

CONTENT = 128
ROTARY = 64
SPAN = 8
LANES = 128
CHUNKS = 4

norm_eps = 1e-06
rope_theta = 10000.0
masked_score = -1e30
MESH = pl.DeviceIdType.MESH


def rms_scale(latent, scaling):
    entries = latent.astype(jnp.float32)
    scaled = entries * lax.rsqrt(jnp.mean(entries * entries, axis=-1, keepdims=True) + norm_eps)
    return (scaled * scaling).astype(jnp.bfloat16)


def kernel(
    sp_size,
    tp_size,
    query_ref,
    shared_ref,
    rotary_ref,
    start_ref,
    query_gain_ref,
    shared_gain_ref,
    frequency_ref,
    content_hbm,
    rotary_hbm,
    key_hbm,
    value_hbm,
    output_hbm,
    mixed_hbm,
    content_w,
    rotary_w,
    key_w,
    value_w,
    output_w,
    halo,
    keys,
    values,
    turns,
    queries,
    query_rows,
    cosines,
    sines,
    bias,
    attended,
    terms,
    landed,
    load_sems,
    halo_recv,
    halo_send,
    term_recv,
    term_send,
    store_sems,
):
    length = query_ref.shape[0]
    shared_rank = shared_ref.shape[1]
    heads = keys.shape[0]
    fold = length * ROTARY // shared_rank
    window = SPAN * length
    rows = length // CHUNKS
    me = lax.axis_index("sp")
    my_tp = lax.axis_index("tp")
    chips = sp_size // 2
    chip = me // 2
    core = me % 2
    odd = chip % 2 == 1
    partner = me + 1 - 2 * core
    beside = me + 2 - 4 * (chip % 2)
    ahead = me + 4
    has_ahead = chip + 2 < chips
    has_behind = chip >= 2

    loads = [
        pltpu.make_async_copy(source, target, load_sems.at[n])
        for n, (source, target) in enumerate(
            (
                (content_hbm, content_w),
                (rotary_hbm, rotary_w),
                (key_hbm, key_w),
                (value_hbm, value_w),
                (output_hbm, output_w),
            )
        )
    ]
    for load in loads:
        load.start()

    barrier = pltpu.get_barrier_semaphore()
    pl.semaphore_signal(barrier, inc=1, device_id={"sp": partner}, device_id_type=MESH)
    pl.semaphore_signal(barrier, inc=1, device_id={"sp": beside}, device_id_type=MESH)
    for step in range(1, tp_size):
        pl.semaphore_signal(
            barrier, inc=1, device_id={"tp": (my_tp + step) % tp_size}, device_id_type=MESH
        )

    @pl.when(has_ahead)
    def _():
        pl.semaphore_signal(barrier, inc=1, device_id={"sp": ahead}, device_id_type=MESH)

    @pl.when(has_behind)
    def _():
        pl.semaphore_signal(barrier, inc=1, device_id={"sp": me - 4}, device_id_type=MESH)

    lane = lax.broadcasted_iota(jnp.int32, (length, LANES), 1)
    first_half = lane % ROTARY < ROTARY // 2
    low_lanes = lane < ROTARY
    places = (me * length + lax.broadcasted_iota(jnp.int32, (length, LANES), 0)).astype(jnp.float32)
    angles = places * frequency_ref[...]
    cosines[...] = jnp.cos(angles)
    sine = jnp.sin(angles)
    sines[...] = jnp.where(first_half, -sine, sine)

    def rotate(entries):
        swapped = jnp.where(
            first_half,
            pltpu.roll(entries, LANES - ROTARY // 2, 1),
            pltpu.roll(entries, ROTARY // 2, 1),
        )
        return entries * cosines[...] + swapped * sines[...]

    halo[0, :length, :] = rms_scale(shared_ref[...], shared_gain_ref[...])
    raw_key = rotary_ref[...].astype(jnp.float32)
    turned = rotate(jnp.concatenate([raw_key, raw_key], axis=1))
    for j in range(shared_rank // LANES):
        upper = turned[2 * j * fold : (2 * j + 1) * fold]
        lower = turned[(2 * j + 1) * fold : (2 * j + 2) * fold]
        halo[0, length:, j * LANES : (j + 1) * LANES] = jnp.where(
            low_lanes[:fold], upper, lower
        ).astype(jnp.bfloat16)

    pl.semaphore_wait(
        barrier, 1 + tp_size + has_ahead.astype(jnp.int32) + has_behind.astype(jnp.int32)
    )

    def send(n, source, target, device):
        return pltpu.make_async_remote_copy(
            src_ref=halo.at[source],
            dst_ref=halo.at[target],
            send_sem=halo_send.at[n],
            recv_sem=halo_recv.at[target],
            device_id={"sp": device},
            device_id_type=MESH,
        )

    even = jnp.logical_not(odd)
    first_core = core == 0
    second_core = core == 1
    have = lambda slot: me >= slot
    sends = [
        (0, has_ahead, send(0, 0, 4, ahead)),
        (0, even, send(1, 0, 2, beside)),
        (0, first_core, send(2, 0, 1, partner)),
        (4, has_behind & has_ahead & (odd | second_core), send(3, 4, 8, ahead)),
        (4, has_behind & even, send(4, 4, 6, beside)),
        (4, has_behind & odd, send(5, 4, 2, beside)),
        (4, has_behind & first_core, send(6, 4, 5, partner)),
        (4, has_behind & second_core, send(7, 4, 3, partner)),
        (2, have(2) & first_core, send(8, 2, 3, partner)),
        (2, have(2) & second_core, send(9, 2, 1, partner)),
        (8, have(8) & odd, send(10, 8, 6, beside)),
        (8, have(8) & second_core, send(11, 8, 7, partner)),
        (6, have(6) & first_core, send(12, 6, 7, partner)),
        (6, have(6) & second_core, send(13, 6, 5, partner)),
    ]

    def start_from(slot):
        for source, condition, copy in sends:
            if source == slot:

                @pl.when(condition)
                def _(copy=copy):
                    copy.start()

    def await_slot(slot):
        expected = have(slot)
        if slot == 8:
            expected = expected & (odd | second_core)

        @pl.when(expected)
        def _():
            pltpu.make_async_copy(halo.at[slot], halo.at[slot], halo_recv.at[slot]).wait()

        if slot < SPAN:

            @pl.when(jnp.logical_not(expected))
            def _():
                halo[slot] = jnp.zeros(halo.shape[1:], halo.dtype)

    def expand(slot):
        base = (SPAN - 1 - slot) * length
        for j in range(shared_rank // LANES):
            piece = halo[slot, length:, j * LANES : (j + 1) * LANES].astype(jnp.float32)
            flipped = pltpu.roll(piece, ROTARY, 1)
            mask = low_lanes[:fold]
            place = base + 2 * j * fold
            turns[place : place + fold, :] = jnp.where(mask, piece, flipped).astype(jnp.bfloat16)
            turns[place + fold : place + 2 * fold, :] = jnp.where(mask, flipped, piece).astype(
                jnp.bfloat16
            )

        def pair(j, carry):
            columns = pl.ds(pl.multiple_of(j * 2 * LANES, 2 * LANES), 2 * LANES)
            block = halo[slot, :length, :]
            for weight, target in ((key_w, keys), (value_w, values)):
                result = jnp.dot(
                    block, weight[:, columns], preferred_element_type=jnp.float32
                ).astype(jnp.bfloat16)
                target[2 * j, base : base + length, :] = result[:, :LANES]
                target[2 * j + 1, base : base + length, :] = result[:, LANES:]
            return carry

        lax.fori_loop(0, heads // 2, pair, 0)

    start_from(0)

    query_rows[...] = rms_scale(query_ref[...], query_gain_ref[...])
    loads[0].wait()
    loads[1].wait()

    def project(j, carry):
        columns = pl.ds(pl.multiple_of(j * 2 * LANES, 2 * LANES), 2 * LANES)
        content = jnp.dot(
            query_rows[...], content_w[:, columns], preferred_element_type=jnp.float32
        ).astype(jnp.bfloat16)
        narrow = pl.ds(pl.multiple_of(j * LANES, LANES), LANES)
        turned = rotate(
            jnp.dot(query_rows[...], rotary_w[:, narrow], preferred_element_type=jnp.float32)
        )
        queries[2 * j, :, :LANES] = content[:, :LANES]
        queries[2 * j + 1, :, :LANES] = content[:, LANES:]
        queries[2 * j, :, LANES:] = jnp.where(low_lanes, turned, 0.0).astype(jnp.bfloat16)
        queries[2 * j + 1, :, LANES:] = jnp.where(low_lanes, 0.0, turned).astype(jnp.bfloat16)
        return carry

    lax.fori_loop(0, heads // 2, project, 0)
    loads[2].wait()
    loads[3].wait()
    expand(0)
    for slot in (4, 2):
        await_slot(slot)
        start_from(slot)
    expand(4)
    await_slot(1)
    expand(2)
    expand(1)
    for slot in (8, 6):
        await_slot(slot)
        start_from(slot)
    expand(6)
    for slot in (3, 5, 7):
        await_slot(slot)
        expand(slot)
    loads[4].wait()

    factor = (CONTENT + ROTARY) ** (-0.5) * 1.4426950408889634
    opening = (me - (SPAN - 1)) * length

    def term_copy(chunk, step):
        place = pl.ds(pl.multiple_of(chunk * rows, rows), rows)
        return pltpu.make_async_remote_copy(
            src_ref=terms.at[place],
            dst_ref=landed.at[step - 1, place],
            send_sem=term_send.at[step - 1, chunk],
            recv_sem=term_recv.at[step - 1, chunk],
            device_id={"tp": (my_tp + step) % tp_size},
            device_id_type=MESH,
        )

    def attend(chunk, carry):
        offset = pl.multiple_of(chunk * rows, rows)
        place = pl.ds(offset, rows)
        key_places = opening + lax.broadcasted_iota(jnp.int32, (rows, window), 1)
        query_places = me * length + offset + lax.broadcasted_iota(jnp.int32, (rows, window), 0)
        visible = (key_places >= start_ref[place, :]) & (key_places <= query_places)
        bias[...] = jnp.where(visible, 0.0, masked_score)

        def one_head(h, inner):
            held = jnp.concatenate([keys[h], turns[...]], axis=1)
            scores = lax.dot_general(
                queries[h, place, :],
                held,
                (((1,), (1,)), ((), ())),
                preferred_element_type=jnp.float32,
            )
            scores = scores + bias[...]
            highest = jnp.max(scores, axis=-1, keepdims=True)
            weights = jnp.exp2((scores - highest) * factor)
            denominator = jnp.sum(weights, axis=-1, keepdims=True)
            summed = jnp.dot(
                weights.astype(jnp.bfloat16), values[h], preferred_element_type=jnp.float32
            )
            attended[:, pl.ds(pl.multiple_of(h * LANES, LANES), LANES)] = (
                summed / denominator
            ).astype(jnp.bfloat16)
            return inner

        lax.fori_loop(0, heads, one_head, 0)
        wide = 4 * LANES

        def output_columns(j, inner):
            columns = pl.ds(pl.multiple_of(j * wide, wide), wide)
            terms[place, columns] = jnp.dot(
                attended[...], output_w[:, columns], preferred_element_type=jnp.float32
            ).astype(jnp.bfloat16)
            return inner

        lax.fori_loop(0, output_w.shape[1] // wide, output_columns, 0)
        for step in range(1, tp_size):
            term_copy(chunk, step).start()
        return carry

    lax.fori_loop(0, CHUNKS, attend, 0)

    def store_copy(chunk):
        place = pl.ds(pl.multiple_of(chunk * rows, rows), rows)
        return pltpu.make_async_copy(landed.at[0, place], mixed_hbm.at[place], store_sems.at[chunk])

    def finish(chunk, carry):
        place = pl.ds(pl.multiple_of(chunk * rows, rows), rows)
        for step in range(1, tp_size):
            term_copy(chunk, step).wait_recv()
        total = terms[place, :].astype(jnp.float32)
        for step in range(1, tp_size):
            total = total + landed[step - 1, place, :].astype(jnp.float32)
        landed[0, place, :] = total.astype(jnp.bfloat16)
        store_copy(chunk).start()
        return carry

    lax.fori_loop(0, CHUNKS, finish, 0)
    for source, condition, copy in sends:

        @pl.when(condition)
        def _(copy=copy):
            copy.wait_send()

    def drain(chunk, carry):
        for step in range(1, tp_size):
            term_copy(chunk, step).wait_send()
        store_copy(chunk).wait()
        return carry

    lax.fori_loop(0, CHUNKS, drain, 0)


def on_device(
    query_latent,
    shared_latent,
    rotary_key,
    document_start,
    query_gain,
    shared_gain,
    content_weight,
    rotary_weight,
    key_weight,
    value_weight,
    output_weight,
):
    length, query_rank = query_latent.shape
    shared_rank = shared_latent.shape[1]
    sp_size = lax.axis_size("sp")
    tp_size = lax.axis_size("tp")
    heads = key_weight.shape[1] // CONTENT
    model = output_weight.shape[1]
    window = SPAN * length
    half = np.arange(0, ROTARY, 2, dtype=np.float32) / np.float32(ROTARY)
    frequency = (1.0 / np.power(np.float32(rope_theta), half)).astype(np.float32)
    frequency = jnp.asarray(np.tile(frequency, LANES // (ROTARY // 2))[None, :])
    fold = length * ROTARY // shared_rank
    low = jnp.bfloat16
    vmem = pl.BlockSpec(memory_space=pltpu.VMEM)
    hbm = pl.BlockSpec(memory_space=pl.ANY)
    return pl.pallas_call(
        functools.partial(kernel, sp_size, tp_size),
        out_shape=jax.ShapeDtypeStruct((length, model), low),
        in_specs=[vmem] * 7 + [hbm] * 5,
        out_specs=hbm,
        scratch_shapes=[
            pltpu.VMEM(content_weight.shape, low),
            pltpu.VMEM(rotary_weight.shape, low),
            pltpu.VMEM(key_weight.shape, low),
            pltpu.VMEM(value_weight.shape, low),
            pltpu.VMEM(output_weight.shape, low),
            pltpu.VMEM((SPAN + 1, length + fold, shared_rank), low),
            pltpu.VMEM((heads, window, LANES), low),
            pltpu.VMEM((heads, window, LANES), low),
            pltpu.VMEM((window, LANES), low),
            pltpu.VMEM((heads, length, 2 * LANES), low),
            pltpu.VMEM((length, query_rank), low),
            pltpu.VMEM((length, LANES), jnp.float32),
            pltpu.VMEM((length, LANES), jnp.float32),
            pltpu.VMEM((length // CHUNKS, window), jnp.float32),
            pltpu.VMEM((length // CHUNKS, heads * LANES), low),
            pltpu.VMEM((length, model), low),
            pltpu.VMEM((max(tp_size - 1, 1), length, model), low),
            pltpu.SemaphoreType.DMA((5,)),
            pltpu.SemaphoreType.DMA((SPAN + 1,)),
            pltpu.SemaphoreType.DMA((14,)),
            pltpu.SemaphoreType.DMA((max(tp_size - 1, 1), CHUNKS)),
            pltpu.SemaphoreType.DMA((max(tp_size - 1, 1), CHUNKS)),
            pltpu.SemaphoreType.DMA((CHUNKS,)),
        ],
        compiler_params=pltpu.CompilerParams(
            collective_id=0, has_side_effects=True, vmem_limit_bytes=60 * 1024 * 1024
        ),
    )(
        query_latent,
        shared_latent,
        rotary_key,
        document_start.reshape(length, 1),
        query_gain.reshape(1, query_rank),
        shared_gain.reshape(1, shared_rank),
        frequency,
        content_weight,
        rotary_weight,
        key_weight,
        value_weight,
        output_weight,
    )


def solution(mesh):
    return jax.shard_map(
        on_device,
        mesh=mesh,
        in_specs=(
            P("sp", None),
            P("sp", None),
            P("sp", None),
            P("sp"),
            P(),
            P(),
            P(None, "tp"),
            P(None, "tp"),
            P(None, "tp"),
            P(None, "tp"),
            P("tp", None),
        ),
        out_specs=P("sp", None),
        check_vma=False,
    )
```

```python
import functools

import jax
import jax.numpy as jnp
import numpy as np
from jax import lax
from jax.experimental import pallas as pl
from jax.experimental.pallas import tpu as pltpu
from jax.sharding import PartitionSpec as P

CONTENT = 128
ROTARY = 64
SPAN = 8
LANES = 128
CHUNKS = 4
PIECES = CHUNKS + 1

norm_eps = 1e-06
rope_theta = 10000.0
masked_score = -1e30
MESH = pl.DeviceIdType.MESH


def rms_scale(latent, scaling):
    entries = latent.astype(jnp.float32)
    scaled = entries * lax.rsqrt(jnp.mean(entries * entries, axis=-1, keepdims=True) + norm_eps)
    return (scaled * scaling).astype(jnp.bfloat16)


def kernel(
    sp_size,
    tp_size,
    query_ref,
    shared_ref,
    rotary_ref,
    start_ref,
    query_gain_ref,
    shared_gain_ref,
    frequency_ref,
    content_hbm,
    rotary_hbm,
    key_hbm,
    value_hbm,
    output_hbm,
    mixed_hbm,
    content_w,
    rotary_w,
    key_w,
    value_w,
    output_w,
    halo,
    keys,
    values,
    turns,
    queries,
    query_rows,
    cosines,
    sines,
    starts,
    bias,
    attended,
    terms,
    landed,
    load_sems,
    halo_recv,
    halo_send,
    term_recv,
    term_send,
    store_sems,
):
    length = query_ref.shape[0]
    shared_rank = shared_ref.shape[1]
    heads = keys.shape[0]
    fold = length * ROTARY // shared_rank
    window = SPAN * length
    rows = length // CHUNKS
    me = lax.axis_index("sp")
    my_tp = lax.axis_index("tp")
    chips = sp_size // 2
    chip = me // 2
    core = me % 2
    odd = chip % 2 == 1
    partner = me + 1 - 2 * core
    beside = me + 2 - 4 * (chip % 2)
    ahead = me + 4
    has_ahead = chip + 2 < chips
    has_behind = chip >= 2

    loads = [
        pltpu.make_async_copy(source, target, load_sems.at[n])
        for n, (source, target) in enumerate(
            (
                (content_hbm, content_w),
                (rotary_hbm, rotary_w),
                (key_hbm, key_w),
                (value_hbm, value_w),
                (output_hbm, output_w),
            )
        )
    ]
    for load in loads:
        load.start()

    barrier = pltpu.get_barrier_semaphore()
    pl.semaphore_signal(barrier, inc=1, device_id={"sp": partner}, device_id_type=MESH)
    pl.semaphore_signal(barrier, inc=1, device_id={"sp": beside}, device_id_type=MESH)
    for step in range(1, tp_size):
        pl.semaphore_signal(
            barrier, inc=1, device_id={"tp": (my_tp + step) % tp_size}, device_id_type=MESH
        )

    @pl.when(has_ahead)
    def _():
        pl.semaphore_signal(barrier, inc=1, device_id={"sp": ahead}, device_id_type=MESH)

    @pl.when(has_behind)
    def _():
        pl.semaphore_signal(barrier, inc=1, device_id={"sp": me - 4}, device_id_type=MESH)

    lane = lax.broadcasted_iota(jnp.int32, (length, LANES), 1)
    first_half = lane % ROTARY < ROTARY // 2
    low_lanes = lane < ROTARY
    places = (me * length + lax.broadcasted_iota(jnp.int32, (length, LANES), 0)).astype(jnp.float32)
    angles = places * frequency_ref[...]
    cosines[...] = jnp.cos(angles)
    sine = jnp.sin(angles)
    sines[...] = jnp.where(first_half, -sine, sine)

    def rotate(entries):
        swapped = jnp.where(
            first_half,
            pltpu.roll(entries, LANES - ROTARY // 2, 1),
            pltpu.roll(entries, ROTARY // 2, 1),
        )
        return entries * cosines[...] + swapped * sines[...]

    halo[0, :length, :] = rms_scale(shared_ref[...], shared_gain_ref[...])
    raw_key = rotary_ref[...].astype(jnp.float32)
    turned = rotate(jnp.transpose(jnp.concatenate([raw_key, raw_key], axis=0)))
    for j in range(shared_rank // LANES):
        upper = turned[2 * j * fold : (2 * j + 1) * fold]
        lower = turned[(2 * j + 1) * fold : (2 * j + 2) * fold]
        halo[0, length:, j * LANES : (j + 1) * LANES] = jnp.where(
            low_lanes[:fold], upper, lower
        ).astype(jnp.bfloat16)

    pl.semaphore_wait(
        barrier, 1 + tp_size + has_ahead.astype(jnp.int32) + has_behind.astype(jnp.int32)
    )

    def send(n, source, target, device):
        return pltpu.make_async_remote_copy(
            src_ref=halo.at[source],
            dst_ref=halo.at[target],
            send_sem=halo_send.at[n],
            recv_sem=halo_recv.at[target],
            device_id={"sp": device},
            device_id_type=MESH,
        )

    even = jnp.logical_not(odd)
    first_core = core == 0
    second_core = core == 1
    have = lambda slot: me >= slot
    sends = [
        (0, has_ahead, send(0, 0, 4, ahead)),
        (0, even, send(1, 0, 2, beside)),
        (0, first_core, send(2, 0, 1, partner)),
        (4, has_behind & has_ahead & (odd | second_core), send(3, 4, 8, ahead)),
        (4, has_behind & even, send(4, 4, 6, beside)),
        (4, has_behind & odd, send(5, 4, 2, beside)),
        (4, has_behind & first_core, send(6, 4, 5, partner)),
        (4, has_behind & second_core, send(7, 4, 3, partner)),
        (2, have(2) & first_core, send(8, 2, 3, partner)),
        (2, have(2) & second_core, send(9, 2, 1, partner)),
        (8, have(8) & odd, send(10, 8, 6, beside)),
        (8, have(8) & second_core, send(11, 8, 7, partner)),
        (6, have(6) & first_core, send(12, 6, 7, partner)),
        (6, have(6) & second_core, send(13, 6, 5, partner)),
    ]

    def start_from(slot):
        for source, condition, copy in sends:
            if source == slot:

                @pl.when(condition)
                def _(copy=copy):
                    copy.start()

    def await_slot(slot):
        expected = have(slot)
        if slot == 8:
            expected = expected & (odd | second_core)

        @pl.when(expected)
        def _():
            pltpu.make_async_copy(halo.at[slot], halo.at[slot], halo_recv.at[slot]).wait()

        if slot < SPAN:

            @pl.when(jnp.logical_not(expected))
            def _():
                halo[slot] = jnp.zeros(halo.shape[1:], halo.dtype)

    def expand(slot):
        base = (SPAN - 1 - slot) * length
        for j in range(shared_rank // LANES):
            piece = halo[slot, length:, j * LANES : (j + 1) * LANES].astype(jnp.float32)
            flipped = pltpu.roll(piece, ROTARY, 1)
            mask = low_lanes[:fold]
            place = base + 2 * j * fold
            turns[place : place + fold, :] = jnp.where(mask, piece, flipped).astype(jnp.bfloat16)
            turns[place + fold : place + 2 * fold, :] = jnp.where(mask, flipped, piece).astype(
                jnp.bfloat16
            )

        def pair(j, carry):
            columns = pl.ds(pl.multiple_of(j * 2 * LANES, 2 * LANES), 2 * LANES)
            block = halo[slot, :length, :]
            for weight, target in ((key_w, keys), (value_w, values)):
                result = jnp.dot(
                    block, weight[:, columns], preferred_element_type=jnp.float32
                ).astype(jnp.bfloat16)
                target[2 * j, base : base + length, :] = result[:, :LANES]
                target[2 * j + 1, base : base + length, :] = result[:, LANES:]
            return carry

        lax.fori_loop(0, heads // 2, pair, 0)

    start_from(0)

    begin = jnp.broadcast_to(start_ref[...].astype(jnp.float32), (LANES, length))
    starts[...] = jnp.transpose(begin).astype(jnp.int32)
    query_rows[...] = rms_scale(query_ref[...], query_gain_ref[...])
    loads[0].wait()
    loads[1].wait()

    def project(j, carry):
        columns = pl.ds(pl.multiple_of(j * 2 * LANES, 2 * LANES), 2 * LANES)
        content = jnp.dot(
            query_rows[...], content_w[:, columns], preferred_element_type=jnp.float32
        ).astype(jnp.bfloat16)
        narrow = pl.ds(pl.multiple_of(j * LANES, LANES), LANES)
        turned = rotate(
            jnp.dot(query_rows[...], rotary_w[:, narrow], preferred_element_type=jnp.float32)
        )
        queries[2 * j, :, :LANES] = content[:, :LANES]
        queries[2 * j + 1, :, :LANES] = content[:, LANES:]
        queries[2 * j, :, LANES:] = jnp.where(low_lanes, turned, 0.0).astype(jnp.bfloat16)
        queries[2 * j + 1, :, LANES:] = jnp.where(low_lanes, 0.0, turned).astype(jnp.bfloat16)
        return carry

    lax.fori_loop(0, heads // 2, project, 0)
    loads[2].wait()
    loads[3].wait()
    expand(0)
    for slot in (4, 2):
        await_slot(slot)
        start_from(slot)
    expand(4)
    await_slot(1)
    expand(2)
    expand(1)
    for slot in (8, 6):
        await_slot(slot)
        start_from(slot)
    expand(6)
    for slot in (3, 5, 7):
        await_slot(slot)
        expand(slot)
    loads[4].wait()

    factor = (CONTENT + ROTARY) ** (-0.5) * 1.4426950408889634
    opening = (me - (SPAN - 1)) * length

    half = rows // 2
    loops = ((0, 2, half, 0), (2, PIECES, rows, rows))

    def place_of(piece, size, shift):
        return pl.ds(pl.multiple_of(piece * size - shift, half), size)

    def term_copy(chunk, step, size, shift):
        place = place_of(chunk, size, shift)
        return pltpu.make_async_remote_copy(
            src_ref=terms.at[place],
            dst_ref=landed.at[step - 1, place],
            send_sem=term_send.at[step - 1, chunk],
            recv_sem=term_recv.at[step - 1, chunk],
            device_id={"tp": (my_tp + step) % tp_size},
            device_id_type=MESH,
        )

    def attend(size, shift, chunk, carry):
        offset = pl.multiple_of(chunk * size - shift, half)
        place = pl.ds(offset, size)
        key_places = opening + lax.broadcasted_iota(jnp.int32, (size, window), 1)
        query_places = me * length + offset + lax.broadcasted_iota(jnp.int32, (size, window), 0)
        visible = (key_places >= starts[place, :1]) & (key_places <= query_places)
        bias[:size, :] = jnp.where(visible, 0.0, masked_score)

        def one_head(h, inner):
            held = jnp.concatenate([keys[h], turns[...]], axis=1)
            scores = lax.dot_general(
                queries[h, place, :],
                held,
                (((1,), (1,)), ((), ())),
                preferred_element_type=jnp.float32,
            )
            scores = scores + bias[:size, :]
            highest = jnp.max(scores, axis=-1, keepdims=True)
            weights = jnp.exp2((scores - highest) * factor)
            denominator = jnp.sum(weights, axis=-1, keepdims=True)
            summed = jnp.dot(
                weights.astype(jnp.bfloat16), values[h], preferred_element_type=jnp.float32
            )
            attended[:size, pl.ds(pl.multiple_of(h * LANES, LANES), LANES)] = (
                summed / denominator
            ).astype(jnp.bfloat16)
            return inner

        lax.fori_loop(0, heads, one_head, 0)
        wide = 4 * LANES

        def output_columns(j, inner):
            columns = pl.ds(pl.multiple_of(j * wide, wide), wide)
            terms[place, columns] = jnp.dot(
                attended[:size, :], output_w[:, columns], preferred_element_type=jnp.float32
            ).astype(jnp.bfloat16)
            return inner

        lax.fori_loop(0, output_w.shape[1] // wide, output_columns, 0)
        for step in range(1, tp_size):
            term_copy(chunk, step, size, shift).start()
        return carry

    for low, high, size, shift in loops:
        lax.fori_loop(low, high, functools.partial(attend, size, shift), 0)

    def store_copy(chunk, size, shift):
        place = place_of(chunk, size, shift)
        return pltpu.make_async_copy(landed.at[0, place], mixed_hbm.at[place], store_sems.at[chunk])

    def finish(size, shift, chunk, carry):
        place = place_of(chunk, size, shift)
        for step in range(1, tp_size):
            term_copy(chunk, step, size, shift).wait_recv()
        total = terms[place, :].astype(jnp.float32)
        for step in range(1, tp_size):
            total = total + landed[step - 1, place, :].astype(jnp.float32)
        landed[0, place, :] = total.astype(jnp.bfloat16)
        store_copy(chunk, size, shift).start()
        return carry

    for low, high, size, shift in loops:
        lax.fori_loop(low, high, functools.partial(finish, size, shift), 0)
    for source, condition, copy in sends:

        @pl.when(condition)
        def _(copy=copy):
            copy.wait_send()

    def drain(size, shift, chunk, carry):
        for step in range(1, tp_size):
            term_copy(chunk, step, size, shift).wait_send()
        store_copy(chunk, size, shift).wait()
        return carry

    for low, high, size, shift in loops:
        lax.fori_loop(low, high, functools.partial(drain, size, shift), 0)


def on_device(
    query_latent,
    shared_latent,
    rotary_key,
    document_start,
    query_gain,
    shared_gain,
    content_weight,
    rotary_weight,
    key_weight,
    value_weight,
    output_weight,
):
    length, query_rank = query_latent.shape
    shared_rank = shared_latent.shape[1]
    sp_size = lax.axis_size("sp")
    tp_size = lax.axis_size("tp")
    heads = key_weight.shape[1] // CONTENT
    model = output_weight.shape[1]
    window = SPAN * length
    half = np.arange(0, ROTARY, 2, dtype=np.float32) / np.float32(ROTARY)
    frequency = (1.0 / np.power(np.float32(rope_theta), half)).astype(np.float32)
    frequency = jnp.asarray(np.tile(frequency, LANES // (ROTARY // 2))[None, :])
    fold = length * ROTARY // shared_rank
    low = jnp.bfloat16
    vmem = pl.BlockSpec(memory_space=pltpu.VMEM)
    hbm = pl.BlockSpec(memory_space=pl.ANY)
    return pl.pallas_call(
        functools.partial(kernel, sp_size, tp_size),
        out_shape=jax.ShapeDtypeStruct((length, model), low),
        in_specs=[vmem] * 7 + [hbm] * 5,
        out_specs=hbm,
        scratch_shapes=[
            pltpu.VMEM(content_weight.shape, low),
            pltpu.VMEM(rotary_weight.shape, low),
            pltpu.VMEM(key_weight.shape, low),
            pltpu.VMEM(value_weight.shape, low),
            pltpu.VMEM(output_weight.shape, low),
            pltpu.VMEM((SPAN + 1, length + fold, shared_rank), low),
            pltpu.VMEM((heads, window, LANES), low),
            pltpu.VMEM((heads, window, LANES), low),
            pltpu.VMEM((window, LANES), low),
            pltpu.VMEM((heads, length, 2 * LANES), low),
            pltpu.VMEM((length, query_rank), low),
            pltpu.VMEM((length, LANES), jnp.float32),
            pltpu.VMEM((length, LANES), jnp.float32),
            pltpu.VMEM((length, LANES), jnp.int32),
            pltpu.VMEM((length // CHUNKS, window), jnp.float32),
            pltpu.VMEM((length // CHUNKS, heads * LANES), low),
            pltpu.VMEM((length, model), low),
            pltpu.VMEM((max(tp_size - 1, 1), length, model), low),
            pltpu.SemaphoreType.DMA((5,)),
            pltpu.SemaphoreType.DMA((SPAN + 1,)),
            pltpu.SemaphoreType.DMA((14,)),
            pltpu.SemaphoreType.DMA((max(tp_size - 1, 1), PIECES)),
            pltpu.SemaphoreType.DMA((max(tp_size - 1, 1), PIECES)),
            pltpu.SemaphoreType.DMA((PIECES,)),
        ],
        compiler_params=pltpu.CompilerParams(
            collective_id=0, has_side_effects=True, vmem_limit_bytes=60 * 1024 * 1024
        ),
    )(
        query_latent,
        shared_latent,
        rotary_key.T,
        document_start.reshape(1, length),
        query_gain.reshape(1, query_rank),
        shared_gain.reshape(1, shared_rank),
        frequency,
        content_weight,
        rotary_weight,
        key_weight,
        value_weight,
        output_weight,
    )


def solution(mesh):
    return jax.shard_map(
        on_device,
        mesh=mesh,
        in_specs=(
            P("sp", None),
            P("sp", None),
            P("sp", None),
            P("sp"),
            P(),
            P(),
            P(None, "tp"),
            P(None, "tp"),
            P(None, "tp"),
            P(None, "tp"),
            P("tp", None),
        ),
        out_specs=P("sp", None),
        check_vma=False,
    )
```

```python
import functools

import jax
import jax.numpy as jnp
import numpy as np
from jax import lax
from jax.experimental import pallas as pl
from jax.experimental.pallas import tpu as pltpu
from jax.sharding import PartitionSpec as P

CONTENT = 128
ROTARY = 64
SPAN = 8
LANES = 128
CHUNKS = 4

norm_eps = 1e-06
rope_theta = 10000.0
masked_score = -1e30
MESH = pl.DeviceIdType.MESH


def rms_scale(latent, scaling):
    entries = latent.astype(jnp.float32)
    scaled = entries * lax.rsqrt(jnp.mean(entries * entries, axis=-1, keepdims=True) + norm_eps)
    return (scaled * scaling).astype(jnp.bfloat16)


def kernel(
    sp_size,
    tp_size,
    query_ref,
    shared_ref,
    rotary_ref,
    start_ref,
    query_gain_ref,
    shared_gain_ref,
    frequency_ref,
    content_hbm,
    rotary_hbm,
    key_hbm,
    value_hbm,
    output_hbm,
    mixed_hbm,
    content_w,
    rotary_w,
    key_w,
    value_w,
    output_w,
    halo,
    keys,
    values,
    turns,
    queries,
    query_rows,
    cosines,
    sines,
    starts,
    bias,
    attended,
    terms,
    landed,
    load_sems,
    halo_recv,
    halo_send,
    term_recv,
    term_send,
    store_sems,
):
    length = query_ref.shape[0]
    shared_rank = shared_ref.shape[1]
    heads = keys.shape[0]
    fold = length * ROTARY // shared_rank
    window = SPAN * length
    rows = length // CHUNKS
    me = lax.axis_index("sp")
    my_tp = lax.axis_index("tp")
    chips = sp_size // 2
    chip = me // 2
    core = me % 2
    odd = chip % 2 == 1
    partner = me + 1 - 2 * core
    beside = me + 2 - 4 * (chip % 2)
    ahead = me + 4
    has_ahead = chip + 2 < chips
    has_behind = chip >= 2

    loads = [
        pltpu.make_async_copy(source, target, load_sems.at[n])
        for n, (source, target) in enumerate(
            (
                (content_hbm, content_w),
                (rotary_hbm, rotary_w),
                (key_hbm, key_w),
                (value_hbm, value_w),
                (output_hbm, output_w),
            )
        )
    ]
    for load in loads:
        load.start()

    barrier = pltpu.get_barrier_semaphore()
    pl.semaphore_signal(barrier, inc=1, device_id={"sp": partner}, device_id_type=MESH)
    pl.semaphore_signal(barrier, inc=1, device_id={"sp": beside}, device_id_type=MESH)
    for step in range(1, tp_size):
        pl.semaphore_signal(
            barrier, inc=1, device_id={"tp": (my_tp + step) % tp_size}, device_id_type=MESH
        )

    @pl.when(has_ahead)
    def _():
        pl.semaphore_signal(barrier, inc=1, device_id={"sp": ahead}, device_id_type=MESH)

    @pl.when(has_behind)
    def _():
        pl.semaphore_signal(barrier, inc=1, device_id={"sp": me - 4}, device_id_type=MESH)

    lane = lax.broadcasted_iota(jnp.int32, (length, LANES), 1)
    first_half = lane % ROTARY < ROTARY // 2
    low_lanes = lane < ROTARY
    places = (me * length + lax.broadcasted_iota(jnp.int32, (length, LANES), 0)).astype(jnp.float32)
    angles = places * frequency_ref[...]
    cosines[...] = jnp.cos(angles)
    sine = jnp.sin(angles)
    sines[...] = jnp.where(first_half, -sine, sine)

    def rotate(entries):
        swapped = jnp.where(
            first_half,
            pltpu.roll(entries, LANES - ROTARY // 2, 1),
            pltpu.roll(entries, ROTARY // 2, 1),
        )
        return entries * cosines[...] + swapped * sines[...]

    halo[0, :length, :] = rms_scale(shared_ref[...], shared_gain_ref[...])
    raw_key = rotary_ref[...].astype(jnp.float32)
    turned = rotate(jnp.transpose(jnp.concatenate([raw_key, raw_key], axis=0)))
    for j in range(shared_rank // LANES):
        upper = turned[2 * j * fold : (2 * j + 1) * fold]
        lower = turned[(2 * j + 1) * fold : (2 * j + 2) * fold]
        halo[0, length:, j * LANES : (j + 1) * LANES] = jnp.where(
            low_lanes[:fold], upper, lower
        ).astype(jnp.bfloat16)

    pl.semaphore_wait(
        barrier, 1 + tp_size + has_ahead.astype(jnp.int32) + has_behind.astype(jnp.int32)
    )

    def send(n, source, target, device):
        return pltpu.make_async_remote_copy(
            src_ref=halo.at[source],
            dst_ref=halo.at[target],
            send_sem=halo_send.at[n],
            recv_sem=halo_recv.at[target],
            device_id={"sp": device},
            device_id_type=MESH,
        )

    even = jnp.logical_not(odd)
    first_core = core == 0
    second_core = core == 1
    have = lambda slot: me >= slot
    sends = [
        (0, has_ahead, send(0, 0, 4, ahead)),
        (0, even, send(1, 0, 2, beside)),
        (0, first_core, send(2, 0, 1, partner)),
        (4, has_behind & has_ahead & (odd | second_core), send(3, 4, 8, ahead)),
        (4, has_behind & even, send(4, 4, 6, beside)),
        (4, has_behind & odd, send(5, 4, 2, beside)),
        (4, has_behind & first_core, send(6, 4, 5, partner)),
        (4, has_behind & second_core, send(7, 4, 3, partner)),
        (2, have(2) & first_core, send(8, 2, 3, partner)),
        (2, have(2) & second_core, send(9, 2, 1, partner)),
        (8, have(8) & odd, send(10, 8, 6, beside)),
        (8, have(8) & second_core, send(11, 8, 7, partner)),
        (6, have(6) & first_core, send(12, 6, 7, partner)),
        (6, have(6) & second_core, send(13, 6, 5, partner)),
    ]

    def start_from(slot):
        for source, condition, copy in sends:
            if source == slot:

                @pl.when(condition)
                def _(copy=copy):
                    copy.start()

    def await_slot(slot):
        expected = have(slot)
        if slot == 8:
            expected = expected & (odd | second_core)

        @pl.when(expected)
        def _():
            pltpu.make_async_copy(halo.at[slot], halo.at[slot], halo_recv.at[slot]).wait()

        if slot < SPAN:

            @pl.when(jnp.logical_not(expected))
            def _():
                halo[slot] = jnp.zeros(halo.shape[1:], halo.dtype)

    def expand(slot):
        base = (SPAN - 1 - slot) * length
        for j in range(shared_rank // LANES):
            piece = halo[slot, length:, j * LANES : (j + 1) * LANES].astype(jnp.float32)
            flipped = pltpu.roll(piece, ROTARY, 1)
            mask = low_lanes[:fold]
            place = base + 2 * j * fold
            turns[place : place + fold, :] = jnp.where(mask, piece, flipped).astype(jnp.bfloat16)
            turns[place + fold : place + 2 * fold, :] = jnp.where(mask, flipped, piece).astype(
                jnp.bfloat16
            )

        def pair(j, carry):
            columns = pl.ds(pl.multiple_of(j * 2 * LANES, 2 * LANES), 2 * LANES)
            block = halo[slot, :length, :]
            for weight, target in ((key_w, keys), (value_w, values)):
                result = jnp.dot(
                    block, weight[:, columns], preferred_element_type=jnp.float32
                ).astype(jnp.bfloat16)
                target[2 * j, base : base + length, :] = result[:, :LANES]
                target[2 * j + 1, base : base + length, :] = result[:, LANES:]
            return carry

        lax.fori_loop(0, heads // 2, pair, 0)

    start_from(0)

    begin = jnp.broadcast_to(start_ref[...].astype(jnp.float32), (LANES, length))
    starts[...] = jnp.transpose(begin).astype(jnp.int32)
    query_rows[...] = rms_scale(query_ref[...], query_gain_ref[...])
    loads[0].wait()
    loads[1].wait()

    def project(j, carry):
        columns = pl.ds(pl.multiple_of(j * 2 * LANES, 2 * LANES), 2 * LANES)
        content = jnp.dot(
            query_rows[...], content_w[:, columns], preferred_element_type=jnp.float32
        ).astype(jnp.bfloat16)
        narrow = pl.ds(pl.multiple_of(j * LANES, LANES), LANES)
        turned = rotate(
            jnp.dot(query_rows[...], rotary_w[:, narrow], preferred_element_type=jnp.float32)
        )
        queries[2 * j, :, :LANES] = content[:, :LANES]
        queries[2 * j + 1, :, :LANES] = content[:, LANES:]
        queries[2 * j, :, LANES:] = jnp.where(low_lanes, turned, 0.0).astype(jnp.bfloat16)
        queries[2 * j + 1, :, LANES:] = jnp.where(low_lanes, 0.0, turned).astype(jnp.bfloat16)
        return carry

    lax.fori_loop(0, heads // 2, project, 0)
    loads[2].wait()
    loads[3].wait()
    expand(0)
    for slot in (4, 2):
        await_slot(slot)
        start_from(slot)
    expand(4)
    await_slot(1)
    expand(2)
    expand(1)
    for slot in (8, 6):
        await_slot(slot)
        start_from(slot)
    expand(6)
    for slot in (3, 5, 7):
        await_slot(slot)
        expand(slot)
    loads[4].wait()

    factor = (CONTENT + ROTARY) ** (-0.5) * 1.4426950408889634
    opening = (me - (SPAN - 1)) * length

    half = rows // 2
    loops = ((0, CHUNKS, rows, 0),)

    def place_of(piece, size, shift):
        return pl.ds(pl.multiple_of(piece * size - shift, half), size)

    def term_copy(chunk, step, size, shift):
        place = place_of(chunk, size, shift)
        return pltpu.make_async_remote_copy(
            src_ref=terms.at[place],
            dst_ref=landed.at[step - 1, place],
            send_sem=term_send.at[step - 1, chunk],
            recv_sem=term_recv.at[step - 1, chunk],
            device_id={"tp": (my_tp + step) % tp_size},
            device_id_type=MESH,
        )

    def attend(size, shift, chunk, carry):
        offset = pl.multiple_of(chunk * size - shift, half)
        place = pl.ds(offset, size)
        key_places = opening + lax.broadcasted_iota(jnp.int32, (size, window), 1)
        query_places = me * length + offset + lax.broadcasted_iota(jnp.int32, (size, window), 0)
        visible = (key_places >= starts[place, :1]) & (key_places <= query_places)
        bias[:size, :] = jnp.where(visible, 0.0, masked_score)

        def one_head(h, inner):
            held = jnp.concatenate([keys[h], turns[...]], axis=1)
            scores = lax.dot_general(
                queries[h, place, :],
                held,
                (((1,), (1,)), ((), ())),
                preferred_element_type=jnp.float32,
            )
            scores = scores + bias[:size, :]
            highest = jnp.max(scores, axis=-1, keepdims=True)
            weights = jnp.exp2((scores - highest) * factor)
            denominator = jnp.sum(weights, axis=-1, keepdims=True)
            summed = jnp.dot(
                weights.astype(jnp.bfloat16), values[h], preferred_element_type=jnp.float32
            )
            attended[:size, pl.ds(pl.multiple_of(h * LANES, LANES), LANES)] = (
                summed / denominator
            ).astype(jnp.bfloat16)
            return inner

        lax.fori_loop(0, heads, one_head, 0, unroll=2)
        wide = 4 * LANES

        def output_columns(j, inner):
            columns = pl.ds(pl.multiple_of(j * wide, wide), wide)
            terms[place, columns] = jnp.dot(
                attended[:size, :], output_w[:, columns], preferred_element_type=jnp.float32
            ).astype(jnp.bfloat16)
            return inner

        lax.fori_loop(0, output_w.shape[1] // wide, output_columns, 0)
        for step in range(1, tp_size):
            term_copy(chunk, step, size, shift).start()
        return carry

    for low, high, size, shift in loops:
        lax.fori_loop(low, high, functools.partial(attend, size, shift), 0)

    def store_copy(chunk, size, shift):
        place = place_of(chunk, size, shift)
        return pltpu.make_async_copy(landed.at[0, place], mixed_hbm.at[place], store_sems.at[chunk])

    def finish(size, shift, chunk, carry):
        place = place_of(chunk, size, shift)
        for step in range(1, tp_size):
            term_copy(chunk, step, size, shift).wait_recv()
        total = terms[place, :].astype(jnp.float32)
        for step in range(1, tp_size):
            total = total + landed[step - 1, place, :].astype(jnp.float32)
        landed[0, place, :] = total.astype(jnp.bfloat16)
        store_copy(chunk, size, shift).start()
        return carry

    for low, high, size, shift in loops:
        lax.fori_loop(low, high, functools.partial(finish, size, shift), 0)
    for source, condition, copy in sends:

        @pl.when(condition)
        def _(copy=copy):
            copy.wait_send()

    def drain(size, shift, chunk, carry):
        for step in range(1, tp_size):
            term_copy(chunk, step, size, shift).wait_send()
        store_copy(chunk, size, shift).wait()
        return carry

    for low, high, size, shift in loops:
        lax.fori_loop(low, high, functools.partial(drain, size, shift), 0)


def on_device(
    query_latent,
    shared_latent,
    rotary_key,
    document_start,
    query_gain,
    shared_gain,
    content_weight,
    rotary_weight,
    key_weight,
    value_weight,
    output_weight,
):
    length, query_rank = query_latent.shape
    shared_rank = shared_latent.shape[1]
    sp_size = lax.axis_size("sp")
    tp_size = lax.axis_size("tp")
    heads = key_weight.shape[1] // CONTENT
    model = output_weight.shape[1]
    window = SPAN * length
    half = np.arange(0, ROTARY, 2, dtype=np.float32) / np.float32(ROTARY)
    frequency = (1.0 / np.power(np.float32(rope_theta), half)).astype(np.float32)
    frequency = jnp.asarray(np.tile(frequency, LANES // (ROTARY // 2))[None, :])
    fold = length * ROTARY // shared_rank
    low = jnp.bfloat16
    vmem = pl.BlockSpec(memory_space=pltpu.VMEM)
    hbm = pl.BlockSpec(memory_space=pl.ANY)
    return pl.pallas_call(
        functools.partial(kernel, sp_size, tp_size),
        out_shape=jax.ShapeDtypeStruct((length, model), low),
        in_specs=[vmem] * 7 + [hbm] * 5,
        out_specs=hbm,
        scratch_shapes=[
            pltpu.VMEM(content_weight.shape, low),
            pltpu.VMEM(rotary_weight.shape, low),
            pltpu.VMEM(key_weight.shape, low),
            pltpu.VMEM(value_weight.shape, low),
            pltpu.VMEM(output_weight.shape, low),
            pltpu.VMEM((SPAN + 1, length + fold, shared_rank), low),
            pltpu.VMEM((heads, window, LANES), low),
            pltpu.VMEM((heads, window, LANES), low),
            pltpu.VMEM((window, LANES), low),
            pltpu.VMEM((heads, length, 2 * LANES), low),
            pltpu.VMEM((length, query_rank), low),
            pltpu.VMEM((length, LANES), jnp.float32),
            pltpu.VMEM((length, LANES), jnp.float32),
            pltpu.VMEM((length, LANES), jnp.int32),
            pltpu.VMEM((length // CHUNKS, window), jnp.float32),
            pltpu.VMEM((length // CHUNKS, heads * LANES), low),
            pltpu.VMEM((length, model), low),
            pltpu.VMEM((max(tp_size - 1, 1), length, model), low),
            pltpu.SemaphoreType.DMA((5,)),
            pltpu.SemaphoreType.DMA((SPAN + 1,)),
            pltpu.SemaphoreType.DMA((14,)),
            pltpu.SemaphoreType.DMA((max(tp_size - 1, 1), CHUNKS)),
            pltpu.SemaphoreType.DMA((max(tp_size - 1, 1), CHUNKS)),
            pltpu.SemaphoreType.DMA((CHUNKS,)),
        ],
        compiler_params=pltpu.CompilerParams(
            collective_id=0, has_side_effects=True, vmem_limit_bytes=60 * 1024 * 1024
        ),
    )(
        query_latent,
        shared_latent,
        rotary_key.T,
        document_start.reshape(1, length),
        query_gain.reshape(1, query_rank),
        shared_gain.reshape(1, shared_rank),
        frequency,
        content_weight,
        rotary_weight,
        key_weight,
        value_weight,
        output_weight,
    )


def solution(mesh):
    return jax.shard_map(
        on_device,
        mesh=mesh,
        in_specs=(
            P("sp", None),
            P("sp", None),
            P("sp", None),
            P("sp"),
            P(),
            P(),
            P(None, "tp"),
            P(None, "tp"),
            P(None, "tp"),
            P(None, "tp"),
            P("tp", None),
        ),
        out_specs=P("sp", None),
        check_vma=False,
    )
```
